32 devices in a mesh: sp: 4 (over z), dp: 8 (over y, x, core).
Axes of the slice: x: 2, y: 2, z: 4, core: 2. Of those that a mesh axis runs over, the one named last changes fastest.
Arguments:
- normed: bfloat16 [8, 1024, 512], P('dp', None, 'sp'), may hold values from -6 to 6
- branch_in: bfloat16 [8, 1024, 512], P('dp', 'sp'), may hold values from -12 to 12
- gate_pre: bfloat16 [8, 1024, 512], P('dp', 'sp'), may hold values from -6 to 6
- cotangent: bfloat16 [8, 1024, 512], P('dp', None, 'sp'), may hold values from -6 to 6
- decay_shift: float32 [8, 16, 512], P('dp', 'sp'), may hold values from -1.2 to -0.000390625
- conv_weight: float32 [4, 1024], P(None, 'sp'), may hold values from -3 to 3
- recur_weight: float32 [16, 64, 64], P('sp'), may hold values from -0.75 to 0.75
- input_weight: float32 [16, 64, 64], P('sp'), may hold values from -0.75 to 0.75
- decay_param: float32 [1024], P('sp')
- branch_proj: bfloat16 [1024, 1024], P('dp'), may hold values from -0.1875 to 0.1875
Outputs:
- grad_normed: bfloat16 [8, 1024, 512], P('dp', None, 'sp')
- grad_gate: bfloat16 [8, 1024, 512], P('dp', 'sp')
- grad_proj: float32 [1024, 1024], P('dp', 'sp')
- grad_conv: float32 [4, 1024], P(None, 'sp')
- grad_recur: float32 [16, 64, 64], P('sp')
- grad_input: float32 [16, 64, 64], P('sp')
- grad_decay: float32 [1024], P('sp')
The draws below stay inside these ranges and needn't reach their ends.
All inputs are finite; a program needn't handle non-finite values.
Results may differ from the reference program's by a relative error of at most 0.019.
Values may be sent and summed in bfloat16 or wider, within the bound.
A program may use at most 64 MiB of HBM per device.

```python
import jax
import jax.numpy as jnp
from jax import lax

D = 1024
REC_BLOCKS = 16
BLOCK_W = 64
CONV = 4
TOK_DEV = 128
D_REC = 1024
LENGTH = 512
SEQS = 8


def draw_branch_in(key, part):
    first, second = jax.random.split(jax.random.fold_in(key, 3))
    spans = LENGTH // TOK_DEV
    factor = jnp.exp(jax.random.uniform(second, (SEQS, 1, spans), jnp.float32, -0.6, 0.6))
    factor = jnp.repeat(factor, TOK_DEV, axis=2)
    values = jax.random.normal(first, (SEQS, D_REC, LENGTH), jnp.float32)
    return (values * factor).astype(jnp.bfloat16)


def draw_decay_shift(key, part):
    first, second, third = jax.random.split(jax.random.fold_in(key, 11), 3)
    spans = LENGTH // TOK_DEV
    base = -jax.random.uniform(first, (SEQS, REC_BLOCKS, spans), jnp.float32, 0.2, 1.0) / LENGTH
    base = jnp.repeat(base, TOK_DEV, axis=2)
    where = jax.random.randint(second, (SEQS, REC_BLOCKS, 2), 0, LENGTH)
    depth = jnp.log(jax.random.uniform(third, (SEQS, REC_BLOCKS, 2), jnp.float32, 0.55, 0.8))
    places = jnp.arange(LENGTH)
    hits = (places[None, None, None, :] == where[:, :, :, None]).astype(jnp.float32)
    return base + jnp.sum(hits * depth[:, :, :, None], axis=2)


def draw_decay_param(key, part):
    first, second, third = jax.random.split(jax.random.fold_in(key, 7), 3)
    share = 0.5
    quick = jax.random.bernoulli(first, share, (D_REC,))
    quick_rate = jnp.exp(jax.random.uniform(second, (D_REC,), jnp.float32, jnp.log(2.5), jnp.log(8.0))) / TOK_DEV
    slow_rate = jnp.exp(jax.random.uniform(third, (D_REC,), jnp.float32, jnp.log(0.1), jnp.log(0.6))) / LENGTH
    softened = jnp.where(quick, quick_rate, slow_rate) / 4.0
    return -jnp.log(jnp.expm1(softened))


def spiked(entries, rng, source, target, parts, factor):
    def block_of(position):
        return (jnp.arange(entries.shape[position]) // (entries.shape[position] // parts)).reshape((-1,) + (1,) * (entries.ndim - 1 - position))

    first = jax.random.permutation(rng, parts)[block_of(target)]
    far = (block_of(target) + parts // 2) % parts
    return jnp.where((block_of(source) == first) | (block_of(source) == far), factor * entries, entries)


def steps_of(rng, extent, pieces, smallest, top_value):
    level = 1.0
    for dim, blocks in pieces:
        steps = jax.random.uniform(jax.random.fold_in(jax.random.fold_in(rng, 6), dim), (blocks,), jnp.float32, smallest / len(pieces), top_value / len(pieces))
        level = level * jnp.repeat(jnp.exp(steps), extent[dim] // blocks).reshape((-1,) + (1,) * (len(extent) - 1 - dim))
    return level


def centred(key, extent, width, reach, shards=(), held_as=jnp.bfloat16):
    entries = width * jax.random.normal(key, extent, jnp.float32)
    if shards:
        entries = entries * steps_of(key, extent, shards, -0.22, 0.18)
    return jnp.clip(entries, -reach, reach).astype(held_as)


def gaussian_with(stream_key, extent, spread, limit, pieces, heavy, dtype=jnp.bfloat16):
    values = spread * jax.random.normal(stream_key, extent, jnp.float32)
    if pieces:
        values = values * steps_of(stream_key, extent, pieces, -0.22, 0.18)
    return jnp.clip(spiked(values, jax.random.fold_in(stream_key, 3), *heavy), -limit, limit).astype(dtype)


def setup_inputs(seed: int = 0) -> dict:
    seeds = jax.random.split(jax.random.key(seed), 11)
    normed = gaussian_with(seeds[0], (SEQS, D, LENGTH), 1.0, 6.0, ((0, 8), (2, 4)), (0, 1, 8, 2.0))
    branch_in = draw_branch_in(jax.random.fold_in(seeds[10], 71), 0)
    gate_pre = centred(seeds[2], (SEQS, D_REC, LENGTH), 1.0, 6.0, ((0, 8), (1, 4)))
    cotangent = gaussian_with(seeds[3], (SEQS, D_REC, LENGTH), 1.0, 6.0, ((0, 8), (2, 4)), (2, 1, 4, 2.0))
    decay_shift = draw_decay_shift(jax.random.fold_in(seeds[10], 71), 0)
    conv_weight = centred(seeds[5], (CONV, D_REC), CONV ** -0.5, 3.0, ((1, 4),), jnp.float32)
    recur_weight = centred(seeds[6], (REC_BLOCKS, BLOCK_W, BLOCK_W), BLOCK_W ** -0.5, 0.75, ((0, 4),), jnp.float32)
    input_weight = centred(seeds[7], (REC_BLOCKS, BLOCK_W, BLOCK_W), BLOCK_W ** -0.5, 0.75, ((0, 4),), jnp.float32)
    decay_param = draw_decay_param(jax.random.fold_in(seeds[10], 71), 0)
    branch_proj = centred(seeds[9], (D, D_REC), D ** -0.5, 0.1875, ((0, 8),))
    return dict(normed=normed, branch_in=branch_in, gate_pre=gate_pre, cotangent=cotangent, decay_shift=decay_shift, conv_weight=conv_weight, recur_weight=recur_weight, input_weight=input_weight, decay_param=decay_param, branch_proj=branch_proj)


gate_const = 8.0
highest = lax.Precision.HIGHEST

def mixer(branch, gate, shift, conv_weight, recur_weight, input_weight, decay_param):
    channels, length = branch.shape
    values = branch.astype(jnp.float32)
    padded = jnp.pad(values, ((0, 0), (CONV - 1, 0)))
    convolved = conv_weight[0][:, None] * padded[:, 0:length]
    for offset in range(1, CONV):
        convolved = convolved + conv_weight[offset][:, None] * padded[:, offset:offset + length]
    groups = channels // BLOCK_W
    grouped = convolved.reshape(groups, BLOCK_W, length)
    recur_gate = jax.nn.sigmoid(jnp.einsum('gil,gij->gjl', grouped, recur_weight, precision=highest).reshape(channels, length))
    input_gate = jax.nn.sigmoid(jnp.einsum('gil,gij->gjl', grouped, input_weight, precision=highest).reshape(channels, length))
    log_decay = -gate_const * recur_gate * jax.nn.softplus(-decay_param)[:, None] + jnp.repeat(shift, BLOCK_W, axis=0)
    decay = jnp.exp(log_decay)
    pushed = jnp.sqrt(-jnp.expm1(2.0 * log_decay)) * input_gate * convolved

    def combine(earlier, later):
        return (earlier[0] * later[0], later[0] * earlier[1] + later[1])
    _, states = lax.associative_scan(combine, (decay, pushed), axis=1)
    return states * jax.nn.gelu(gate.astype(jnp.float32))

def mixer_grads(branch, gate, shift, upstream, conv_weight, recur_weight, input_weight, decay_param):

    def local(branch_f, gate_f, conv_f, recur_f, input_f, decay_f):
        return mixer(branch_f, gate_f, shift, conv_f, recur_f, input_f, decay_f)
    _, pullback = jax.vjp(local, branch.astype(jnp.float32), gate.astype(jnp.float32), conv_weight, recur_weight, input_weight, decay_param)
    return pullback(upstream.astype(jnp.float32))

def reference(normed, branch_in, gate_pre, cotangent, decay_shift, conv_weight, recur_weight, input_weight, decay_param, branch_proj):

    def per_sequence(carry, items):
        seq_normed, seq_branch, seq_gate, seq_cot, seq_shift = items
        grad_branch, grad_gate, grad_conv, grad_recur, grad_input, grad_decay = mixer_grads(seq_branch, seq_gate, seq_shift, seq_cot, conv_weight, recur_weight, input_weight, decay_param)
        branch_rounded = grad_branch.astype(jnp.bfloat16)
        grad_normed = jnp.dot(branch_proj, branch_rounded, preferred_element_type=jnp.float32).astype(jnp.bfloat16)
        proj_term = lax.dot_general(seq_normed, branch_rounded, (((1,), (1,)), ((), ())), preferred_element_type=jnp.float32)
        carry = (carry[0] + proj_term, carry[1] + grad_conv, carry[2] + grad_recur, carry[3] + grad_input, carry[4] + grad_decay)
        return (carry, (grad_normed, grad_gate.astype(jnp.bfloat16)))
    start = (jnp.zeros((D, D_REC), jnp.float32), jnp.zeros((CONV, D_REC), jnp.float32), jnp.zeros((REC_BLOCKS, BLOCK_W, BLOCK_W), jnp.float32), jnp.zeros((REC_BLOCKS, BLOCK_W, BLOCK_W), jnp.float32), jnp.zeros((D_REC,), jnp.float32))
    totals, outputs = lax.scan(per_sequence, start, (normed, branch_in, gate_pre, cotangent, decay_shift))
    return (outputs[0], outputs[1], totals[0], totals[1], totals[2], totals[3], totals[4])
```

```python
import functools

import jax
import jax.numpy as jnp
from jax import lax
from jax.experimental import pallas as pl
from jax.experimental.pallas import tpu as pltpu
from jax.sharding import PartitionSpec as P

BLOCK_W = 64
CONV = 4
GATE = 8.0
LANES = 128
GELU_C = 0.7978845608028654
GELU_K = 0.044715
f32 = jnp.float32
bf16 = jnp.bfloat16


def lane_ids():
    return lax.broadcasted_iota(jnp.int32, (BLOCK_W, LANES), 1)


def shift_right(chunks, k, lane):
    rolled = [pltpu.roll(c, k, 1) for c in chunks]
    out = []
    for q in range(len(chunks)):
        before = rolled[q - 1] if q else jnp.zeros_like(rolled[0])
        out.append(jnp.where(lane >= k, rolled[q], before))
    return out


def shift_left(chunks, k, lane):
    n = len(chunks)
    rolled = [pltpu.roll(c, LANES - k, 1) for c in chunks]
    out = []
    for q in range(n):
        after = rolled[q + 1] if q + 1 < n else jnp.zeros_like(rolled[0])
        out.append(jnp.where(lane < LANES - k, rolled[q], after))
    return out


def scan_right(decay, pushed, lane):
    spans = []
    for a, u in zip(decay, pushed):
        k = 1
        while k < LANES:
            keep = lane >= k
            u = u + a * jnp.where(keep, pltpu.roll(u, k, 1), 0.0)
            a = a * jnp.where(keep, pltpu.roll(a, k, 1), 1.0)
            k *= 2
        spans.append((a, u))
    out = []
    carry = None
    for a, u in spans:
        h = u if carry is None else u + a * carry
        carry = h[:, LANES - 1 : LANES]
        out.append(h)
    return out


def scan_left(decay, pushed, lane):
    spans = []
    for a, u in zip(decay, pushed):
        k = 1
        while k < LANES:
            keep = lane < LANES - k
            u = u + a * jnp.where(keep, pltpu.roll(u, LANES - k, 1), 0.0)
            a = a * jnp.where(keep, pltpu.roll(a, LANES - k, 1), 1.0)
            k *= 2
        spans.append((a, u))
    out = []
    carry = None
    for a, u in reversed(spans):
        h = u if carry is None else u + a * carry
        carry = h[:, 0:1]
        out.append(h)
    return out[::-1]


def softplus_neg(p):
    z = jnp.exp(-jnp.abs(p))
    y = z / (2.0 + z)
    y2 = y * y
    poly = jnp.full_like(y, 1.0 / 19.0)
    for d in (17, 15, 13, 11, 9, 7, 5, 3):
        poly = poly * y2 + 1.0 / d
    poly = poly * y2 + 1.0
    return jnp.maximum(-p, 0.0) + 2.0 * y * poly


def sigmoid(v):
    return 1.0 / (1.0 + jnp.exp(-v))


def dot(a, b, dims):
    return lax.dot_general(a, b, (dims, ((), ())), preferred_element_type=f32)


def split(v):
    hi = v.astype(bf16)
    lo = (v - hi.astype(f32)).astype(bf16)
    return hi, lo


def kernel(
    nsp,
    ndp,
    normed_ref,
    branch_ref,
    gate_ref,
    cot_ref,
    shift_ref,
    conv_ref,
    recur_ref,
    input_ref,
    decay_ref,
    proj_ref,
    gn_ref,
    gg_ref,
    gproj_ref,
    gconv_ref,
    grecur_ref,
    ginput_ref,
    gdecay_ref,
    cot_all,
    norm_all,
    proj_all,
    tok_all,
    part_all,
    part_send,
    small_all,
    cd_all,
    gb,
    small_send,
    cd_send,
    cdf,
    cols,
    gcols,
    xs,
    rs,
    gs,
    as_,
    ivs,
    hs,
    cot_s,
    cot_r,
    norm_s,
    norm_r,
    proj_s,
    proj_r,
    fwd_s,
    fwd_r,
    tok_s,
    tok_r,
    part_s,
    part_r,
    small_s,
    small_r,
    cd_s,
    cd_r,
    local_sem,
):
    me_s = lax.axis_index("sp")
    me_d = lax.axis_index("dp")
    chan = branch_ref.shape[1]
    groups = chan // BLOCK_W
    width = normed_ref.shape[1]
    rows_here = proj_ref.shape[0]
    MESH = pl.DeviceIdType.MESH

    def sp_peer(k):
        return lax.rem(me_s + k, nsp)

    def dp_peer(k):
        return lax.rem(me_d + k, ndp)

    sibling = me_d + 1 - 2 * lax.rem(me_d, 2)

    def remote(src, dst, ss, rs_, device):
        return pltpu.make_async_remote_copy(
            src_ref=src, dst_ref=dst, send_sem=ss, recv_sem=rs_,
            device_id=device, device_id_type=MESH,
        )

    own = [
        pltpu.make_async_copy(
            cot_ref.at[0, pl.ds(me_s * chan, chan), :], cot_all.at[me_s], local_sem.at[0]
        ),
        pltpu.make_async_copy(normed_ref.at[0], norm_all.at[me_s], local_sem.at[1]),
        pltpu.make_async_copy(proj_ref, proj_all.at[me_d], local_sem.at[2]),
    ]
    for c in own:
        c.start()

    barrier = pltpu.get_barrier_semaphore()
    for k in range(1, nsp):
        pl.semaphore_signal(barrier, inc=1, device_id={"sp": sp_peer(k)}, device_id_type=MESH)
    for k in range(1, ndp):
        pl.semaphore_signal(barrier, inc=1, device_id={"dp": dp_peer(k)}, device_id_type=MESH)
    pl.semaphore_wait(barrier, nsp - 1 + ndp - 1)

    cot_copies = []
    for k in range(1, nsp):
        to = sp_peer(k)
        cot_copies.append(
            remote(
                cot_ref.at[0, pl.ds(to * chan, chan), :], cot_all.at[me_s],
                cot_s.at[k], cot_r.at[k], {"sp": to},
            )
        )
    for c in cot_copies:
        c.start()
    proj_copies = [
        remote(proj_ref, proj_all.at[me_d], proj_s.at[k], proj_r.at[k], {"dp": dp_peer(k)})
        for k in range(2, ndp, 2)
    ]
    proj_copies.append(
        remote(proj_ref, proj_all.at[me_d], proj_s.at[0], proj_r.at[0], {"dp": sibling})
    )
    norm_copies = [
        remote(
            normed_ref.at[0], norm_all.at[me_s], norm_s.at[k], norm_r.at[k], {"sp": sp_peer(k)}
        )
        for k in range(1, nsp)
    ]
    for c in norm_copies + proj_copies:
        c.start()

    lane = lane_ids()
    eye = lax.broadcasted_iota(jnp.int32, (chan, chan), 0) == lax.broadcasted_iota(
        jnp.int32, (chan, chan), 1
    )
    params = [conv_ref[k : k + 1, :] for k in range(CONV)] + [
        -GATE * softplus_neg(decay_ref[...])
    ]
    for k, row in enumerate(params):
        cols[k] = jnp.sum(jnp.where(eye, row, 0.0), axis=1, keepdims=True)

    @pl.loop(0, groups)
    def _(g):
        rows = pl.ds(pl.multiple_of(g * BLOCK_W, BLOCK_W), BLOCK_W)
        b = [
            branch_ref[0, rows, q * LANES : (q + 1) * LANES].astype(f32) for q in range(nsp)
        ]
        x = [cols[CONV - 1, rows, :] * v for v in b]
        for m in range(1, CONV):
            w = cols[CONV - 1 - m, rows, :]
            x = [v + w * s for v, s in zip(x, shift_right(b, m, lane))]
        x_full = jnp.concatenate(x, axis=1)
        hi, lo = split(x_full)
        x3 = jnp.concatenate([hi, lo, hi], axis=0)
        gates = []
        for ref in (recur_ref, input_ref):
            whi, wlo = split(ref[g])
            w3 = jnp.concatenate([whi, whi, wlo], axis=0)
            gates.append(sigmoid(dot(w3, x3, ((0,), (0,)))))
        rate = cols[CONV, rows, :]
        of_group = lax.broadcasted_iota(jnp.int32, (groups, LANES), 0) == g
        decays, pushes = [], []
        for q in range(nsp):
            span = slice(q * LANES, (q + 1) * LANES)
            r = gates[0][:, span]
            i = gates[1][:, span]
            shift = jnp.where(of_group, shift_ref[0, :, span], 0.0)
            logs = rate * r + jnp.sum(shift, axis=0, keepdims=True)
            y = 2.0 * logs
            a = jnp.exp(logs)
            rest = jnp.where(
                y > -0.02, -y * (1.0 + y * (0.5 + y * (1.0 / 6.0))), 1.0 - a * a
            )
            inv = lax.rsqrt(rest)
            decays.append(a)
            pushes.append(rest * inv * i * x[q])
            xs[q, rows, :] = x[q]
            rs[q, rows, :] = r
            gs[q, rows, :] = i
            as_[q, rows, :] = a
            ivs[q, rows, :] = inv
        for q, h in enumerate(scan_right(decays, pushes, lane)):
            hs[q, rows, :] = h

    own[0].wait()
    for c in cot_copies:
        c.wait()

    @pl.loop(0, groups)
    def _(g):
        rows = pl.ds(pl.multiple_of(g * BLOCK_W, BLOCK_W), BLOCK_W)
        a = [as_[q, rows, :] for q in range(nsp)]
        h = [hs[q, rows, :] for q in range(nsp)]
        direct = []
        for q in range(nsp):
            span = slice(q * LANES, (q + 1) * LANES)
            z = gate_ref[0, rows, span].astype(f32)
            cot = cot_all[q, rows, :].astype(f32)
            z2 = z * z
            th = jnp.tanh(GELU_C * z * (1.0 + GELU_K * z2))
            half = 0.5 * (1.0 + th)
            slope = half + 0.5 * z * (1.0 - th * th) * (
                GELU_C * (1.0 + 3.0 * GELU_K * z2)
            )
            direct.append(cot * z * half)
            gg_ref[0, rows, span] = (cot * h[q] * slope).astype(bf16)
        lam = scan_left(shift_left(a, 1, lane), direct, lane)
        before = shift_right(h, 1, lane)
        rate = cols[CONV, rows, :]
        dx, drz, diz = [], [], []
        ddecay = jnp.zeros((BLOCK_W, LANES), f32)
        for q in range(nsp):
            x = xs[q, rows, :]
            r = rs[q, rows, :]
            i = gs[q, rows, :]
            inv = ivs[q, rows, :]
            scale = (1.0 - a[q] * a[q]) * inv
            scale = jnp.where(a[q] > 0.99, 1.0 / inv, scale)
            ix = i * x
            dlog = lam[q] * a[q] * (before[q] - ix * a[q] * inv)
            ls = lam[q] * scale
            dx.append(ls * i)
            diz.append(ls * ix * (1.0 - i))
            rl = dlog * r
            ddecay = ddecay + rl
            drz.append(rl * rate * (1.0 - r))
        gcols[CONV, rows, :] = -GATE * jnp.sum(ddecay, axis=1, keepdims=True)
        drz_b = jnp.concatenate(drz, axis=1).astype(bf16)
        diz_b = jnp.concatenate(diz, axis=1).astype(bf16)
        x_b = jnp.concatenate([xs[q, rows, :] for q in range(nsp)], axis=1).astype(bf16)
        small_send[g] = dot(
            x_b, jnp.concatenate([drz_b, diz_b], axis=0), ((1,), (1,))
        ).astype(bf16)
        through = dot(recur_ref[g].astype(bf16), drz_b, ((1,), (0,))) + dot(
            input_ref[g].astype(bf16), diz_b, ((1,), (0,))
        )
        dx = [v + through[:, q * LANES : (q + 1) * LANES] for q, v in enumerate(dx)]
        b = [
            branch_ref[0, rows, q * LANES : (q + 1) * LANES].astype(f32) for q in range(nsp)
        ]
        db = [cols[CONV - 1, rows, :] * v for v in dx]
        for m in range(CONV):
            w = cols[CONV - 1 - m, rows, :]
            bm = shift_right(b, m, lane) if m else b
            total = dx[0] * bm[0]
            for q in range(1, nsp):
                total = total + dx[q] * bm[q]
            gcols[CONV - 1 - m, rows, :] = jnp.sum(total, axis=1, keepdims=True)
            if m:
                db = [v + w * s for v, s in zip(db, shift_left(dx, m, lane))]
        for q in range(nsp):
            gb[q, rows, :] = db[q].astype(bf16)

    tok_copies = []
    for k in range(1, nsp):
        to = sp_peer(k)
        tok_copies.append(
            remote(gb.at[to], tok_all.at[me_s], tok_s.at[k], tok_r.at[k], {"sp": to})
        )
    for c in tok_copies:
        c.start()
    tok_all[me_s] = gb[me_s]

    fwd_copies = []
    for c in proj_copies:
        c.wait()
    for k in range(2, ndp, 2):
        src = lax.rem(me_d + ndp - k, ndp)
        fwd_copies.append(
            remote(proj_all.at[src], proj_all.at[src], fwd_s.at[k], fwd_r.at[k], {"dp": sibling})
        )
    for c in fwd_copies:
        c.start()

    own[1].wait()
    for c in norm_copies:
        c.wait()
    gb_full = jnp.concatenate([gb[q] for q in range(nsp)], axis=1)
    part_copies = []
    for k in list(range(1, ndp)) + [0]:
        to = dp_peer(k)
        block = pl.ds(pl.multiple_of(to * rows_here, rows_here), rows_here)
        lhs = jnp.concatenate([norm_all[q, block, :] for q in range(nsp)], axis=1)
        term = dot(lhs, gb_full, ((1,), (1,)))
        if k == 0:
            part_all[me_d] = term.astype(bf16)
            continue
        part_send[k] = term.astype(bf16)
        c = remote(
            part_send.at[k], part_all.at[me_d], part_s.at[k], part_r.at[k], {"dp": to}
        )
        c.start()
        part_copies.append(c)

    cdf[...] = jnp.zeros_like(cdf)
    for k in range(CONV + 1):
        row = jnp.sum(jnp.where(eye, gcols[k], 0.0), axis=0, keepdims=True)
        if k == CONV:
            row = -row * sigmoid(-decay_ref[...])
        cdf[k : k + 1, :] = row
    cd_send[...] = cdf[...].astype(bf16)
    small_copies = []
    for k in range(1, ndp):
        to = {"dp": dp_peer(k)}
        small_copies.append(
            remote(small_send, small_all.at[me_d], small_s.at[k], small_r.at[k], to)
        )
        small_copies.append(remote(cd_send, cd_all.at[me_d], cd_s.at[k], cd_r.at[k], to))
    for c in small_copies:
        c.start()
    small_all[me_d] = small_send[...]
    cd_all[me_d] = cd_send[...]

    own[2].wait()
    for c in fwd_copies + tok_copies:
        c.wait()
    tokens = tok_all[...].reshape(nsp * chan, LANES)
    per = max(1, min(ndp, 256 // rows_here))
    for j in range(0, ndp, per):
        lhs = proj_all[j : j + per].reshape(per * rows_here, nsp * chan)
        gn_ref[0, j * rows_here : (j + per) * rows_here, :] = dot(
            lhs, tokens, ((1,), (0,))
        ).astype(bf16)

    for c in part_copies:
        c.wait()
    total = part_all[0].astype(f32)
    for j in range(1, ndp):
        total = total + part_all[j].astype(f32)
    gproj_ref[...] = total
    for c in small_copies:
        c.wait()
    total = small_all[0].astype(f32)
    for j in range(1, ndp):
        total = total + small_all[j].astype(f32)
    grecur_ref[...] = total[:, :, :BLOCK_W]
    ginput_ref[...] = total[:, :, BLOCK_W:]
    total = cd_all[0].astype(f32)
    for j in range(1, ndp):
        total = total + cd_all[j].astype(f32)
    gconv_ref[...] = total[:CONV, :]
    gdecay_ref[...] = total[CONV : CONV + 1, :]


def body(
    normed, branch_in, gate_pre, cotangent, decay_shift,
    conv_weight, recur_weight, input_weight, decay_param, branch_proj,
):
    nsp = lax.axis_size("sp")
    ndp = lax.axis_size("dp")
    chan, length = branch_in.shape[1:]
    width, span = normed.shape[1:]
    groups = chan // BLOCK_W
    rows = branch_proj.shape[0]
    vmem = pl.BlockSpec(memory_space=pltpu.VMEM)
    hbm = pl.BlockSpec(memory_space=pl.ANY)
    V = pltpu.VMEM
    dma = lambda n: pltpu.SemaphoreType.DMA((n,))
    state = V((nsp, chan, LANES), f32)
    out = pl.pallas_call(
        functools.partial(kernel, nsp, ndp),
        out_shape=(
            jax.ShapeDtypeStruct((1, width, span), bf16),
            jax.ShapeDtypeStruct((1, chan, length), bf16),
            jax.ShapeDtypeStruct((rows, chan), f32),
            jax.ShapeDtypeStruct((CONV, chan), f32),
            jax.ShapeDtypeStruct((groups, BLOCK_W, BLOCK_W), f32),
            jax.ShapeDtypeStruct((groups, BLOCK_W, BLOCK_W), f32),
            jax.ShapeDtypeStruct((1, chan), f32),
        ),
        in_specs=[hbm, vmem, vmem, hbm, vmem, vmem, vmem, vmem, vmem, hbm],
        out_specs=[vmem] * 7,
        scratch_shapes=[
            V((nsp, chan, LANES), bf16),
            V((nsp, width, LANES), bf16),
            V((ndp, rows, nsp * chan), bf16),
            V((nsp, chan, LANES), bf16),
            V((ndp, rows, chan), bf16),
            V((ndp, rows, chan), bf16),
            V((ndp, groups, BLOCK_W, 2 * BLOCK_W), bf16),
            V((ndp, 16, chan), bf16),
            V((nsp, chan, LANES), bf16),
            V((groups, BLOCK_W, 2 * BLOCK_W), bf16),
            V((16, chan), bf16),
            V((16, chan), f32),
            V((CONV + 1, chan, 1), f32),
            V((CONV + 1, chan, 1), f32),
            state, state, state, state, state, state,
            dma(nsp), dma(nsp), dma(nsp), dma(nsp),
            dma(ndp), dma(ndp), dma(ndp), dma(ndp),
            dma(nsp), dma(nsp),
            dma(ndp), dma(ndp), dma(ndp), dma(ndp), dma(ndp), dma(ndp),
            dma(3),
        ],
        compiler_params=pltpu.CompilerParams(
            collective_id=0, has_side_effects=True, vmem_limit_bytes=60000 * 1024
        ),
    )(
        normed, branch_in, gate_pre, cotangent, decay_shift,
        conv_weight, recur_weight, input_weight, decay_param.reshape(1, chan), branch_proj,
    )
    return out[:6] + (out[6].reshape(chan),)


def solution(mesh):
    return jax.shard_map(
        body,
        mesh=mesh,
        in_specs=(
            P("dp", None, "sp"),
            P("dp", "sp", None),
            P("dp", "sp", None),
            P("dp", None, "sp"),
            P("dp", "sp", None),
            P(None, "sp"),
            P("sp", None, None),
            P("sp", None, None),
            P("sp"),
            P("dp", None),
        ),
        out_specs=(
            P("dp", None, "sp"),
            P("dp", "sp", None),
            P("dp", "sp"),
            P(None, "sp"),
            P("sp", None, None),
            P("sp", None, None),
            P("sp"),
        ),
        check_vma=False,
    )
```

```python
import functools

import jax
import jax.numpy as jnp
from jax import lax
from jax.experimental import pallas as pl
from jax.experimental.pallas import tpu as pltpu
from jax.sharding import PartitionSpec as P

BLOCK_W = 64
CONV = 4
GATE = 8.0
LANES = 128
GELU_C = 0.7978845608028654
GELU_K = 0.044715
f32 = jnp.float32
bf16 = jnp.bfloat16


def lane_ids():
    return lax.broadcasted_iota(jnp.int32, (BLOCK_W, LANES), 1)


def shift_right(chunks, k, lane):
    rolled = [pltpu.roll(c, k, 1) for c in chunks]
    out = []
    for q in range(len(chunks)):
        before = rolled[q - 1] if q else jnp.zeros_like(rolled[0])
        out.append(jnp.where(lane >= k, rolled[q], before))
    return out


def shift_left(chunks, k, lane):
    n = len(chunks)
    rolled = [pltpu.roll(c, LANES - k, 1) for c in chunks]
    out = []
    for q in range(n):
        after = rolled[q + 1] if q + 1 < n else jnp.zeros_like(rolled[0])
        out.append(jnp.where(lane < LANES - k, rolled[q], after))
    return out


def scan_right(decay, pushed, lane):
    spans = []
    for a, u in zip(decay, pushed):
        k = 1
        while k < LANES:
            keep = lane >= k
            u = u + a * jnp.where(keep, pltpu.roll(u, k, 1), 0.0)
            a = a * jnp.where(keep, pltpu.roll(a, k, 1), 1.0)
            k *= 2
        spans.append((a, u))
    out = []
    carry = None
    for a, u in spans:
        h = u if carry is None else u + a * carry
        carry = h[:, LANES - 1 : LANES]
        out.append(h)
    return out


def scan_left(decay, pushed, lane):
    spans = []
    for a, u in zip(decay, pushed):
        k = 1
        while k < LANES:
            keep = lane < LANES - k
            u = u + a * jnp.where(keep, pltpu.roll(u, LANES - k, 1), 0.0)
            a = a * jnp.where(keep, pltpu.roll(a, LANES - k, 1), 1.0)
            k *= 2
        spans.append((a, u))
    out = []
    carry = None
    for a, u in reversed(spans):
        h = u if carry is None else u + a * carry
        carry = h[:, 0:1]
        out.append(h)
    return out[::-1]


def softplus_neg(p):
    z = jnp.exp(-jnp.abs(p))
    y = z / (2.0 + z)
    y2 = y * y
    poly = jnp.full_like(y, 1.0 / 19.0)
    for d in (17, 15, 13, 11, 9, 7, 5, 3):
        poly = poly * y2 + 1.0 / d
    poly = poly * y2 + 1.0
    return jnp.maximum(-p, 0.0) + 2.0 * y * poly


def sigmoid(v):
    return 1.0 / (1.0 + jnp.exp(-v))


def dot(a, b, dims):
    return lax.dot_general(a, b, (dims, ((), ())), preferred_element_type=f32)


def split(v):
    hi = v.astype(bf16)
    lo = (v - hi.astype(f32)).astype(bf16)
    return hi, lo


def kernel(
    nsp,
    ndp,
    normed_ref,
    branch_ref,
    gate_ref,
    cot_ref,
    shift_ref,
    conv_ref,
    recur_ref,
    input_ref,
    decay_ref,
    proj_ref,
    gn_ref,
    gg_ref,
    gproj_ref,
    gconv_ref,
    grecur_ref,
    ginput_ref,
    gdecay_ref,
    cot_all,
    norm_all,
    proj_all,
    tok_all,
    part_all,
    part_send,
    small_all,
    cd_all,
    gb,
    small_send,
    cd_send,
    cdf,
    cols,
    gcols,
    xs,
    rs,
    gs,
    as_,
    ivs,
    hs,
    cot_s,
    cot_r,
    norm_s,
    norm_r,
    proj_s,
    proj_r,
    fwd_s,
    fwd_r,
    tok_s,
    tok_r,
    part_s,
    part_r,
    small_s,
    small_r,
    cd_s,
    cd_r,
    local_sem,
):
    me_s = lax.axis_index("sp")
    me_d = lax.axis_index("dp")
    chan = branch_ref.shape[1]
    groups = chan // BLOCK_W
    width = normed_ref.shape[1]
    rows_here = proj_ref.shape[0]
    MESH = pl.DeviceIdType.MESH

    def sp_peer(k):
        return lax.rem(me_s + k, nsp)

    def dp_peer(k):
        return lax.rem(me_d + k, ndp)

    sibling = me_d + 1 - 2 * lax.rem(me_d, 2)

    def remote(src, dst, ss, rs_, device):
        return pltpu.make_async_remote_copy(
            src_ref=src, dst_ref=dst, send_sem=ss, recv_sem=rs_,
            device_id=device, device_id_type=MESH,
        )

    own = [
        pltpu.make_async_copy(
            cot_ref.at[0, pl.ds(me_s * chan, chan), :], cot_all.at[me_s], local_sem.at[0]
        ),
        pltpu.make_async_copy(normed_ref.at[0], norm_all.at[me_s], local_sem.at[1]),
        pltpu.make_async_copy(proj_ref, proj_all.at[me_d], local_sem.at[2]),
    ]
    for c in own:
        c.start()

    barrier = pltpu.get_barrier_semaphore()
    for k in range(1, nsp):
        pl.semaphore_signal(barrier, inc=1, device_id={"sp": sp_peer(k)}, device_id_type=MESH)
    for k in range(1, ndp):
        pl.semaphore_signal(barrier, inc=1, device_id={"dp": dp_peer(k)}, device_id_type=MESH)
    pl.semaphore_wait(barrier, nsp - 1 + ndp - 1)

    cot_copies = []
    for k in range(1, nsp):
        to = sp_peer(k)
        cot_copies.append(
            remote(
                cot_ref.at[0, pl.ds(to * chan, chan), :], cot_all.at[me_s],
                cot_s.at[k], cot_r.at[k], {"sp": to},
            )
        )
    for c in cot_copies:
        c.start()
    proj_copies = [
        remote(proj_ref, proj_all.at[me_d], proj_s.at[k], proj_r.at[k], {"dp": dp_peer(k)})
        for k in range(2, ndp, 2)
    ]
    proj_copies.append(
        remote(proj_ref, proj_all.at[me_d], proj_s.at[0], proj_r.at[0], {"dp": sibling})
    )
    order = list(range(1, ndp)) + [0]

    def block_of(k):
        return pl.ds(pl.multiple_of(dp_peer(k) * rows_here, rows_here), rows_here)

    norm_copies = {
        k: [
            remote(
                normed_ref.at[0, block_of(k), :], norm_all.at[me_s, block_of(k), :],
                norm_s.at[k, j], norm_r.at[k, j], {"sp": sp_peer(j)},
            )
            for j in range(1, nsp)
        ]
        for k in order
    }
    for k in order:
        for c in norm_copies[k]:
            c.start()
    for c in proj_copies:
        c.start()

    lane = lane_ids()
    eye = lax.broadcasted_iota(jnp.int32, (chan, chan), 0) == lax.broadcasted_iota(
        jnp.int32, (chan, chan), 1
    )
    params = [conv_ref[k : k + 1, :] for k in range(CONV)] + [
        -GATE * softplus_neg(decay_ref[...])
    ]
    for k, row in enumerate(params):
        cols[k] = jnp.sum(jnp.where(eye, row, 0.0), axis=1, keepdims=True)

    @pl.loop(0, groups)
    def _(g):
        rows = pl.ds(pl.multiple_of(g * BLOCK_W, BLOCK_W), BLOCK_W)
        b = [
            branch_ref[0, rows, q * LANES : (q + 1) * LANES].astype(f32) for q in range(nsp)
        ]
        x = [cols[CONV - 1, rows, :] * v for v in b]
        for m in range(1, CONV):
            w = cols[CONV - 1 - m, rows, :]
            x = [v + w * s for v, s in zip(x, shift_right(b, m, lane))]
        x_full = jnp.concatenate(x, axis=1)
        hi, lo = split(x_full)
        x3 = jnp.concatenate([hi, lo, hi], axis=0)
        gates = []
        for ref in (recur_ref, input_ref):
            whi, wlo = split(ref[g])
            w3 = jnp.concatenate([whi, whi, wlo], axis=0)
            gates.append(sigmoid(dot(w3, x3, ((0,), (0,)))))
        rate = cols[CONV, rows, :]
        of_group = lax.broadcasted_iota(jnp.int32, (groups, LANES), 0) == g
        decays, pushes = [], []
        for q in range(nsp):
            span = slice(q * LANES, (q + 1) * LANES)
            r = gates[0][:, span]
            i = gates[1][:, span]
            shift = jnp.where(of_group, shift_ref[0, :, span], 0.0)
            logs = rate * r + jnp.sum(shift, axis=0, keepdims=True)
            y = 2.0 * logs
            a = jnp.exp(logs)
            rest = jnp.where(
                y > -0.02, -y * (1.0 + y * (0.5 + y * (1.0 / 6.0))), 1.0 - a * a
            )
            inv = lax.rsqrt(rest)
            decays.append(a)
            pushes.append(rest * inv * i * x[q])
            xs[q, rows, :] = x[q]
            rs[q, rows, :] = r
            gs[q, rows, :] = i
            as_[q, rows, :] = a
            ivs[q, rows, :] = inv
        for q, h in enumerate(scan_right(decays, pushes, lane)):
            hs[q, rows, :] = h

    own[0].wait()
    for c in cot_copies:
        c.wait()
    @pl.loop(0, groups)
    def _(g):
        rows = pl.ds(pl.multiple_of(g * BLOCK_W, BLOCK_W), BLOCK_W)
        a = [as_[q, rows, :] for q in range(nsp)]
        h = [hs[q, rows, :] for q in range(nsp)]
        direct = []
        for q in range(nsp):
            span = slice(q * LANES, (q + 1) * LANES)
            z = gate_ref[0, rows, span].astype(f32)
            cot = cot_all[q, rows, :].astype(f32)
            z2 = z * z
            th = jnp.tanh(GELU_C * z * (1.0 + GELU_K * z2))
            half = 0.5 * (1.0 + th)
            slope = half + 0.5 * z * (1.0 - th * th) * (
                GELU_C * (1.0 + 3.0 * GELU_K * z2)
            )
            direct.append(cot * z * half)
            gg_ref[0, rows, span] = (cot * h[q] * slope).astype(bf16)
        lam = scan_left(shift_left(a, 1, lane), direct, lane)
        before = shift_right(h, 1, lane)
        rate = cols[CONV, rows, :]
        dx, drz, diz = [], [], []
        ddecay = jnp.zeros((BLOCK_W, LANES), f32)
        for q in range(nsp):
            x = xs[q, rows, :]
            r = rs[q, rows, :]
            i = gs[q, rows, :]
            inv = ivs[q, rows, :]
            scale = (1.0 - a[q] * a[q]) * inv
            scale = jnp.where(a[q] > 0.99, 1.0 / inv, scale)
            ix = i * x
            dlog = lam[q] * a[q] * (before[q] - ix * a[q] * inv)
            ls = lam[q] * scale
            dx.append(ls * i)
            diz.append(ls * ix * (1.0 - i))
            rl = dlog * r
            ddecay = ddecay + rl
            drz.append(rl * rate * (1.0 - r))
        gcols[CONV, rows, :] = -GATE * jnp.sum(ddecay, axis=1, keepdims=True)
        drz_b = jnp.concatenate(drz, axis=1).astype(bf16)
        diz_b = jnp.concatenate(diz, axis=1).astype(bf16)
        x_b = jnp.concatenate([xs[q, rows, :] for q in range(nsp)], axis=1).astype(bf16)
        small_send[g] = dot(
            x_b, jnp.concatenate([drz_b, diz_b], axis=0), ((1,), (1,))
        ).astype(bf16)
        through = dot(recur_ref[g].astype(bf16), drz_b, ((1,), (0,))) + dot(
            input_ref[g].astype(bf16), diz_b, ((1,), (0,))
        )
        dx = [v + through[:, q * LANES : (q + 1) * LANES] for q, v in enumerate(dx)]
        b = [
            branch_ref[0, rows, q * LANES : (q + 1) * LANES].astype(f32) for q in range(nsp)
        ]
        db = [cols[CONV - 1, rows, :] * v for v in dx]
        for m in range(CONV):
            w = cols[CONV - 1 - m, rows, :]
            bm = shift_right(b, m, lane) if m else b
            total = dx[0] * bm[0]
            for q in range(1, nsp):
                total = total + dx[q] * bm[q]
            gcols[CONV - 1 - m, rows, :] = jnp.sum(total, axis=1, keepdims=True)
            if m:
                db = [v + w * s for v, s in zip(db, shift_left(dx, m, lane))]
        for q in range(nsp):
            gb[q, rows, :] = db[q].astype(bf16)

    tok_copies = []
    for k in range(1, nsp):
        to = sp_peer(k)
        tok_copies.append(
            remote(gb.at[to], tok_all.at[me_s], tok_s.at[k], tok_r.at[k], {"sp": to})
        )
    for c in tok_copies:
        c.start()
    tok_all[me_s] = gb[me_s]

    small_copies = []
    for k in range(1, ndp):
        to = {"dp": dp_peer(k)}
        small_copies.append(
            remote(small_send, small_all.at[me_d], small_s.at[k], small_r.at[k], to)
        )
    for c in small_copies:
        c.start()
    small_all[me_d] = small_send[...]
    cdf[...] = jnp.zeros_like(cdf)
    for k in range(CONV + 1):
        row = jnp.sum(jnp.where(eye, gcols[k], 0.0), axis=0, keepdims=True)
        if k == CONV:
            row = -row * sigmoid(-decay_ref[...])
        cdf[k : k + 1, :] = row
    cd_send[...] = cdf[...].astype(bf16)
    cd_copies = []
    for k in range(1, ndp):
        to = {"dp": dp_peer(k)}
        cd_copies.append(remote(cd_send, cd_all.at[me_d], cd_s.at[k], cd_r.at[k], to))
    for c in cd_copies:
        c.start()
    cd_all[me_d] = cd_send[...]

    fwd_copies = []
    for c in proj_copies:
        c.wait()
    for k in range(2, ndp, 2):
        src = lax.rem(me_d + ndp - k, ndp)
        fwd_copies.append(
            remote(proj_all.at[src], proj_all.at[src], fwd_s.at[k], fwd_r.at[k], {"dp": sibling})
        )
    for c in fwd_copies:
        c.start()

    own[1].wait()
    gb_full = jnp.concatenate([gb[q] for q in range(nsp)], axis=1)
    part_copies = []
    for k in order:
        to = dp_peer(k)
        block = block_of(k)
        for c in norm_copies[k]:
            c.wait()
        lhs = jnp.concatenate([norm_all[q, block, :] for q in range(nsp)], axis=1)
        term = dot(lhs, gb_full, ((1,), (1,)))
        if k == 0:
            part_all[me_d] = term.astype(bf16)
            continue
        part_send[k] = term.astype(bf16)
        c = remote(
            part_send.at[k], part_all.at[me_d], part_s.at[k], part_r.at[k], {"dp": to}
        )
        c.start()
        part_copies.append(c)

    own[2].wait()
    for c in fwd_copies + tok_copies:
        c.wait()
    tokens = tok_all[...].reshape(nsp * chan, LANES)
    per = max(1, min(ndp, 256 // rows_here))
    for j in range(0, ndp, per):
        lhs = proj_all[j : j + per].reshape(per * rows_here, nsp * chan)
        gn_ref[0, j * rows_here : (j + per) * rows_here, :] = dot(
            lhs, tokens, ((1,), (0,))
        ).astype(bf16)

    for c in small_copies + cd_copies:
        c.wait()
    total = small_all[0].astype(f32)
    for j in range(1, ndp):
        total = total + small_all[j].astype(f32)
    grecur_ref[...] = total[:, :, :BLOCK_W]
    ginput_ref[...] = total[:, :, BLOCK_W:]
    total = cd_all[0].astype(f32)
    for j in range(1, ndp):
        total = total + cd_all[j].astype(f32)
    gconv_ref[...] = total[:CONV, :]
    gdecay_ref[...] = total[CONV : CONV + 1, :]
    for c in part_copies:
        c.wait()
    total = part_all[0].astype(f32)
    for j in range(1, ndp):
        total = total + part_all[j].astype(f32)
    gproj_ref[...] = total


def write_out(*refs):
    count = len(refs) // 2
    for src, dst in zip(refs[:count], refs[count:]):
        dst[...] = src[...]


def body(
    normed, branch_in, gate_pre, cotangent, decay_shift,
    conv_weight, recur_weight, input_weight, decay_param, branch_proj,
):
    nsp = lax.axis_size("sp")
    ndp = lax.axis_size("dp")
    chan, length = branch_in.shape[1:]
    width, span = normed.shape[1:]
    groups = chan // BLOCK_W
    rows = branch_proj.shape[0]
    vmem = pl.BlockSpec(memory_space=pltpu.VMEM)
    hbm = pl.BlockSpec(memory_space=pl.ANY)
    V = pltpu.VMEM
    dma = lambda *n: pltpu.SemaphoreType.DMA(n)
    state = V((nsp, chan, LANES), f32)
    out = pl.pallas_call(
        functools.partial(kernel, nsp, ndp),
        out_shape=(
            jax.ShapeDtypeStruct((1, width, span), bf16),
            jax.ShapeDtypeStruct((1, chan, length), bf16),
            jax.ShapeDtypeStruct((rows, chan), f32),
            jax.ShapeDtypeStruct((CONV, chan), f32),
            jax.ShapeDtypeStruct((groups, BLOCK_W, BLOCK_W), f32),
            jax.ShapeDtypeStruct((groups, BLOCK_W, BLOCK_W), f32),
            jax.ShapeDtypeStruct((1, chan), f32),
        ),
        in_specs=[hbm, vmem, vmem, hbm, vmem, vmem, vmem, vmem, vmem, hbm],
        out_specs=[vmem] * 7,
        scratch_shapes=[
            V((nsp, chan, LANES), bf16),
            V((nsp, width, LANES), bf16),
            V((ndp, rows, nsp * chan), bf16),
            V((nsp, chan, LANES), bf16),
            V((ndp, rows, chan), bf16),
            V((ndp, rows, chan), bf16),
            V((ndp, groups, BLOCK_W, 2 * BLOCK_W), bf16),
            V((ndp, 16, chan), bf16),
            V((nsp, chan, LANES), bf16),
            V((groups, BLOCK_W, 2 * BLOCK_W), bf16),
            V((16, chan), bf16),
            V((16, chan), f32),
            V((CONV + 1, chan, 1), f32),
            V((CONV + 1, chan, 1), f32),
            state, state, state, state, state, state,
            dma(nsp), dma(nsp), dma(ndp, nsp), dma(ndp, nsp),
            dma(ndp), dma(ndp), dma(ndp), dma(ndp),
            dma(nsp), dma(nsp),
            dma(ndp), dma(ndp), dma(ndp), dma(ndp), dma(ndp), dma(ndp),
            dma(3),
        ],
        compiler_params=pltpu.CompilerParams(
            collective_id=0, has_side_effects=True, vmem_limit_bytes=60000 * 1024
        ),
    )(
        normed, branch_in, gate_pre, cotangent, decay_shift,
        conv_weight, recur_weight, input_weight, decay_param.reshape(1, chan), branch_proj,
    )
    out = pl.pallas_call(
        write_out,
        out_shape=tuple(jax.ShapeDtypeStruct(o.shape, o.dtype) for o in out),
        in_specs=[vmem] * 7,
        out_specs=[vmem] * 7,
    )(*out)
    return tuple(out[:6]) + (out[6].reshape(chan),)


def solution(mesh):
    return jax.shard_map(
        body,
        mesh=mesh,
        in_specs=(
            P("dp", None, "sp"),
            P("dp", "sp", None),
            P("dp", "sp", None),
            P("dp", None, "sp"),
            P("dp", "sp", None),
            P(None, "sp"),
            P("sp", None, None),
            P("sp", None, None),
            P("sp"),
            P("dp", None),
        ),
        out_specs=(
            P("dp", None, "sp"),
            P("dp", "sp", None),
            P("dp", "sp"),
            P(None, "sp"),
            P("sp", None, None),
            P("sp", None, None),
            P("sp"),
        ),
        check_vma=False,
    )
```
